32 devices in a mesh: sp: 8 (over z, y), tp: 4 (over x, core).
Axes of the slice: x: 2, y: 2, z: 4, core: 2. Of those that a mesh axis runs over, the one named last changes fastest.
Arguments:
- stream: bfloat16 [2048, 2048], P('sp', 'tp'), may hold values from -1200 to 1200, as said below
- mix_gain: bfloat16 [2048], P('tp'), may hold values from 0.099609375 to 1.8984375
- pool_weight: bfloat16 [4, 512, 512], P('tp'), may hold values from -0.25 to 0.25
- pool_scale: bfloat16 [2048], P('tp'), may hold values from 0.099609375 to 1.8984375
- ffn_gain: bfloat16 [2048], replicated, may hold values from 0.099609375 to 1.8984375
- routes: int32 [2048, 2], P(('sp', 'tp')), may hold values from 0 to 7, all different within a row; in each aligned block of 64 rows (0 to 63, 64 to 127, ...) at most 32 rows name the same one
- route_weight: float32 [2048, 2], P(('sp', 'tp')), may hold values from 0.1 to 1
- w_gate: bfloat16 [8, 2048, 7168], P('sp', None, 'tp'), may hold values from -0.125 to 0.125
- w_up: bfloat16 [8, 2048, 7168], P('sp', None, 'tp'), may hold values from -0.125 to 0.125
- w_down: bfloat16 [8, 7168, 2048], P('sp', 'tp'), may hold values from -0.0625 to 0.0625
Outputs:
- layer_out: bfloat16 [2048, 2048], P(('sp', 'tp'))
The draws below stay inside these ranges and needn't reach their ends.
Inputs may be any that keep to these rules, and one draw needn't show every extreme that they name: `routes`: each row names 2 different experts. Within each aligned block of 64 rows (the rows of one device) no expert is named by more than 32 rows, a bound that some block reaches. `stream`: finite values.
All inputs are finite; a program needn't handle non-finite values.
Results may differ from the reference program's by a relative error of at most 0.0061.
Values may be sent and summed in bfloat16 or wider, within the bound.
A program may use at most 128 MiB of HBM per device.

```python
import math
import jax
import jax.numpy as jnp
import numpy as np
from jax import lax

D = 2048
GROUPS = 4
FF = 7168
TOP = 2
GROUP_W = 512
TQ = 64
EXPERTS = 8
CAP = 32
TOKENS = 2048
N_SP = 8
N_TP = 4


def draw_stream(key, part):
    key_base = jax.random.fold_in(key, 11)
    key_cols = jax.random.fold_in(key, 12)
    base_draw = jnp.clip(jax.random.normal(key_base, (TOKENS, D), jnp.float32), -6.0, 6.0)
    col_scale = jnp.exp(jax.random.uniform(key_cols, (D,), jnp.float32) * math.log(10.0))
    group_index = (jnp.arange(D) // (D // GROUPS)).astype(jnp.float32)
    rise = 3.0 ** (group_index / (GROUPS - 1))
    values = base_draw / 8.0
    return (values * col_scale * rise).astype(jnp.bfloat16)


def block_scale(rng, extent, split, least, top_value):
    level = 1.0
    for dim, blocks in split:
        heights = jax.random.uniform(jax.random.fold_in(jax.random.fold_in(rng, 6), dim), (blocks,), jnp.float32, least / len(split), top_value / len(split))
        level = level * jnp.repeat(jnp.exp(heights), extent[dim] // blocks).reshape((-1,) + (1,) * (len(extent) - 1 - dim))
    return level


def deal_out(stream_key, own, number, rows, amount, top, bound, slope):
    ranking = jax.random.permutation(stream_key, amount)
    heavy_load, usual = portions_of(amount, rows * top, bound, slope, True), portions_of(amount, rows * top, bound, slope, False)
    places = jnp.arange(amount)

    def named(sizes, turn):
        used = int((sizes > 0).sum())
        fixed = max(1, used // 4)
        passed = fixed + (places - fixed + turn * (used - fixed)) % max(1, amount - fixed)
        return jnp.zeros((amount,), jnp.int32).at[ranking[jnp.where(places < fixed, places, passed)]].set(jnp.asarray(sizes, jnp.int32))

    sizes = jnp.where(number % 4 == 0, named(heavy_load, number // 4), named(usual, number - number // 4 - 1))
    mixed = jax.random.permutation(jax.random.fold_in(own, 3), amount)
    donor, receiver = mixed[0:amount // 2 * 2:2], mixed[1:amount // 2 * 2:2]
    slack = jnp.minimum(sizes[donor] - 1, bound - sizes[receiver]) // 2
    slack = jnp.where((donor == ranking[0]) | (receiver == ranking[0]) | (sizes[receiver] == 0), 0, jnp.maximum(slack, 0))
    passed = jax.random.randint(jax.random.fold_in(own, 4), (amount // 2,), 0, 1 << 20) % (slack + 1)
    sizes = sizes.at[donor].add(-passed).at[receiver].add(passed)
    members = jnp.searchsorted(jnp.cumsum(sizes), jnp.arange(rows * top), side="right").astype(jnp.int32)
    table = members.reshape(top, rows).T
    table = table[jax.random.permutation(jax.random.fold_in(own, 1), rows)]
    turn = jax.random.randint(jax.random.fold_in(own, 2), (rows, 1), 0, top)
    return jnp.take_along_axis(table, (jnp.arange(top)[None, :] + turn) % top, axis=1)


def portions_of(amount, total, bound, skew, full):
    portions = [(1 << 20) // math.isqrt(rank ** skew) + 1 for rank in range(1, amount + 1)]
    largest = bound if full else min(bound, max(-(-total // amount), total * portions[0] // sum(portions)))
    least = 1 if total - largest >= amount - 1 else 0
    given, rest = [largest] + [least] * (amount - 1), total - largest - least * (amount - 1)
    while rest > 0:
        free = [i for i in range(1, amount) if given[i] < largest] or [i for i in range(1, amount) if given[i] < bound]
        mass, left = sum([portions[i] for i in free]), rest
        for i in free:
            extra = min(bound - given[i], max(1, left * portions[i] // mass), rest)
            given[i] = given[i] + extra
            rest = rest - extra
    return np.array(given)


def gaussian(key, extent, spread, bound, shards=(), held_as=jnp.bfloat16):
    drawn = jax.random.normal(key, extent, jnp.float32) * spread
    if len(shards) > 0:
        drawn = block_scale(key, extent, shards, -0.22, 0.18) * drawn
    return jnp.clip(drawn, min=-bound, max=bound).astype(held_as)


def setup_inputs(seed: int = 0) -> dict:
    seeds = jax.random.split(jax.random.key(seed), 11)
    stream = draw_stream(jax.random.fold_in(seeds[10], 71), 0)
    mix_gain = jnp.clip(1.0 + 0.18 * jax.random.normal(seeds[1], (D,), jnp.float32), 0.099609375, 1.8984375).astype(jnp.bfloat16)
    pool_weight = gaussian(seeds[2], (GROUPS, GROUP_W, GROUP_W), GROUP_W ** -0.5, 0.25, ((0, 4),))
    pool_scale = jnp.clip(1.0 + 0.18 * jax.random.normal(seeds[3], (D,), jnp.float32), 0.099609375, 1.8984375).astype(jnp.bfloat16)
    ffn_gain = jnp.clip(1.0 + 0.18 * jax.random.normal(seeds[4], (D,), jnp.float32), 0.099609375, 1.8984375).astype(jnp.bfloat16)
    routes_keys = jax.random.split(jax.random.fold_in(seeds[5], 1), TOKENS // TQ)
    routes_turns = jax.random.permutation(jax.random.fold_in(seeds[5], 3), TOKENS // TQ)
    routes = jax.vmap(lambda own, number: deal_out(jax.random.fold_in(seeds[5], 2), own, number, TQ, EXPERTS, TOP, CAP, 1))(routes_keys, routes_turns).reshape((TOKENS, TOP))
    route_weight = jnp.clip(0.1 + 0.9 * jax.random.uniform(seeds[6], (TOKENS, TOP), jnp.float32) ** block_scale(seeds[6], (TOKENS, TOP), ((0, 32),), -0.2, 0.2), 0.1, 1.0)
    w_gate = gaussian(seeds[7], (EXPERTS, D, FF), D ** -0.5, 0.125, ((0, 8), (2, 4)))
    w_up = gaussian(seeds[8], (EXPERTS, D, FF), D ** -0.5, 0.125, ((0, 8), (2, 4)))
    w_down = gaussian(seeds[9], (EXPERTS, FF, D), FF ** -0.5, 0.0625, ((0, 8), (1, 4)))
    return dict(stream=stream, mix_gain=mix_gain, pool_weight=pool_weight, pool_scale=pool_scale, ffn_gain=ffn_gain, routes=routes, route_weight=route_weight, w_gate=w_gate, w_up=w_up, w_down=w_down)


NORM_EPS = 1e-06

def rms_norm(values, gain):
    row_scale = lax.rsqrt(lax.optimization_barrier(jnp.mean(values * values, axis=-1, keepdims=True)) + NORM_EPS)
    return (values * row_scale * gain.astype(jnp.float32)).astype(jnp.bfloat16)

def reference(stream, mix_gain, pool_weight, pool_scale, ffn_gain, routes, route_weight, w_gate, w_up, w_down):
    stream_f32 = stream.astype(jnp.float32)
    normed = rms_norm(stream_f32, mix_gain)
    normed_f32 = normed.astype(jnp.float32)
    group_width = D // GROUPS
    position = jnp.arange(1, TOKENS + 1).astype(jnp.float32)[:, None]
    group_outs = []
    for group_index in range(GROUPS):
        window_len = 2 ** (group_index + 1)
        columns = normed_f32[:, group_index * group_width:(group_index + 1) * group_width]
        window_sum = jnp.zeros_like(columns)
        for lag_rows in range(window_len):
            shifted = jnp.concatenate([jnp.zeros((lag_rows, group_width), jnp.float32), columns[:TOKENS - lag_rows]], axis=0)
            window_sum = window_sum + shifted
        pooled = (window_sum / jnp.minimum(position, jnp.float32(window_len)) - columns).astype(jnp.bfloat16)
        group_outs.append(jnp.dot(pooled, pool_weight[group_index], preferred_element_type=jnp.float32))
    mixer_out = jnp.concatenate(group_outs, axis=1) * pool_scale.astype(jnp.float32)
    after_mix = (stream_f32 + mixer_out).astype(jnp.bfloat16)
    after_f32 = after_mix.astype(jnp.float32)
    normed2 = rms_norm(after_f32, ffn_gain)
    flat_routes = routes.reshape(-1)
    flat_weight = route_weight.reshape(-1)
    max_rows = N_SP * N_TP * CAP
    ff_shard = FF // N_TP

    def one_expert(layer_sum, expert):
        chosen = flat_routes == expert
        picked = jnp.nonzero(chosen, size=max_rows, fill_value=0)[0].astype(jnp.int32)
        is_valid = (jnp.arange(max_rows) < jnp.sum(chosen.astype(jnp.int32))).astype(jnp.float32)
        token_index = picked // TOP
        expert_rows = normed2[token_index]
        gate_val = jnp.dot(expert_rows, w_gate[expert], preferred_element_type=jnp.float32)
        up_val = jnp.dot(expert_rows, w_up[expert], preferred_element_type=jnp.float32)
        hidden = (jax.nn.silu(gate_val) * up_val).astype(jnp.bfloat16)
        summed = jnp.zeros((max_rows, D), jnp.float32)
        for shard_index in range(N_TP):
            block_out = jnp.dot(hidden[:, shard_index * ff_shard:(shard_index + 1) * ff_shard], w_down[expert, shard_index * ff_shard:(shard_index + 1) * ff_shard], preferred_element_type=jnp.float32).astype(jnp.bfloat16)
            summed = summed + lax.optimization_barrier(block_out).astype(jnp.float32)
        expert_out = lax.optimization_barrier(summed.astype(jnp.bfloat16)).astype(jnp.float32)
        weight = flat_weight[picked] * is_valid
        layer_sum = layer_sum.at[token_index].add(weight[:, None] * expert_out)
        return (layer_sum, None)
    expert_total, unused = lax.scan(one_expert, jnp.zeros((TOKENS, D), jnp.float32), jnp.arange(EXPERTS).astype(jnp.int32))
    return (after_f32 + expert_total).astype(jnp.bfloat16)
```

```python
import functools

import jax
import jax.numpy as jnp
from jax import lax
from jax.experimental import pallas as pl
from jax.experimental.pallas import tpu as pltpu
from jax.sharding import PartitionSpec as P

NORM_EPS = 1e-06


def passed_along(block, axis, distance):
    devices = range(lax.axis_size(axis))
    route = [(i - distance, i) for i in devices if i - distance in devices]
    return lax.ppermute(block, axis, route)


MESH = pl.DeviceIdType.MESH
COL_TILE = 256
LANES = 2


def as_rows(block):
    width = block.shape[-1]
    if block.shape[-2] % 16:
        return block.astype(jnp.float32).reshape(-1, width).astype(block.dtype)
    return block.reshape(-1, width)


def col_tile(width):
    return COL_TILE if width % COL_TILE == 0 else width


def expert_kernel(
    sp_count,
    tp_count,
    chunks,
    send_ref,
    pick_ref,
    weight_ref,
    after_ref,
    gate_hbm,
    up_hbm,
    down_hbm,
    out_ref,
    gate,
    up,
    down,
    arrived,
    hidden,
    partial,
    pair_in,
    pair_sum,
    side_in,
    served,
    returned,
    local_sem,
    first_send,
    first_recv,
    side_send,
    side_recv,
    pair_send,
    pair_recv,
    back_pair,
    back_side,
    back_send,
    back_recv,
):
    me = lax.axis_index("sp")
    tp_me = lax.axis_index("tp")
    high, low = tp_me // LANES, lax.rem(tp_me, LANES)
    highs = tp_count // LANES
    other_low = 1 - low
    pair_id = {"sp": me, "tp": high * LANES + other_low}
    steps = sp_count // chunks
    cap, width = send_ref.shape[1:]
    ff_width = gate.shape[1]

    def side_high(distance):
        return lax.rem(high + distance, highs)

    def side_id(distance):
        return {"sp": me, "tp": side_high(distance) * LANES + low}

    def from_high(distance):
        return lax.rem(high - distance + highs, highs)

    weight_copies = [
        pltpu.make_async_copy(source.at[0], target, local_sem.at[index])
        for index, (source, target) in enumerate(((gate_hbm, gate), (up_hbm, up), (down_hbm, down)))
    ]
    own_copy = pltpu.make_async_copy(send_ref.at[0], arrived.at[0, low, high], local_sem.at[3])
    own_copy.start()

    barrier = pltpu.get_barrier_semaphore()
    for step in range(1, sp_count):
        pl.semaphore_signal(
            barrier,
            inc=1,
            device_id={"sp": lax.rem(me + step, sp_count), "tp": tp_me},
            device_id_type=MESH,
        )
    for distance in range(1, highs):
        pl.semaphore_signal(barrier, inc=1, device_id=side_id(distance), device_id_type=MESH)
    pl.semaphore_signal(barrier, inc=1, device_id=pair_id, device_id_type=MESH)
    pl.semaphore_wait(barrier, sp_count - 1 + highs - 1 + 1)

    def first_copy(step):
        return pltpu.make_async_remote_copy(
            src_ref=send_ref.at[step],
            dst_ref=arrived.at[step, low, high],
            send_sem=first_send.at[step],
            recv_sem=first_recv.at[step],
            device_id={"sp": lax.rem(me + step, sp_count), "tp": tp_me},
            device_id_type=MESH,
        )

    def side_copy(step, distance):
        return pltpu.make_async_remote_copy(
            src_ref=arrived.at[step, low, high],
            dst_ref=arrived.at[step, low, high],
            send_sem=side_send.at[step, distance - 1],
            recv_sem=side_recv.at[step, distance - 1],
            device_id=side_id(distance),
            device_id_type=MESH,
        )

    def pair_copy(step, distance):
        block = arrived.at[step, low, from_high(distance)]
        return pltpu.make_async_remote_copy(
            src_ref=block,
            dst_ref=block,
            send_sem=pair_send.at[step, distance],
            recv_sem=pair_recv.at[step, distance],
            device_id=pair_id,
            device_id_type=MESH,
        )

    def chunk_steps(chunk):
        return range(chunk * steps, (chunk + 1) * steps)

    def spread(chunk):
        for step in chunk_steps(chunk):
            if step == 0:
                own_copy.wait()
            else:
                first_copy(step).wait_recv()
            for distance in range(1, highs):
                side_copy(step, distance).start()
            pair_copy(step, 0).start()

    def pass_on(chunk):
        for step in chunk_steps(chunk):
            for distance in range(1, highs):
                side_copy(step, distance).wait_recv()
                pair_copy(step, distance).start()

    def settle(chunk):
        for step in chunk_steps(chunk):
            for distance in range(highs):
                pair_copy(step, distance).wait_recv()

    def span(chunk):
        return pl.ds(chunk * steps, steps)

    def gate_up(chunk):
        tile = col_tile(ff_width)

        def body(index, carry):
            columns = pl.ds(pl.multiple_of(index * tile, tile), tile)
            rows = as_rows(arrived[span(chunk)])
            gate_val = jnp.dot(rows, gate[:, columns], preferred_element_type=jnp.float32)
            up_val = jnp.dot(rows, up[:, columns], preferred_element_type=jnp.float32)
            hidden[:, columns] = (jax.nn.silu(gate_val) * up_val).astype(jnp.bfloat16)
            return carry

        lax.fori_loop(0, ff_width // tile, body, 0)

    def project(chunk):
        tile = col_tile(width)

        def body(index, carry):
            columns = pl.ds(pl.multiple_of(index * tile, tile), tile)
            block = jnp.dot(hidden[...], down[:, columns], preferred_element_type=jnp.float32)
            block = block.reshape(steps, LANES, highs, cap, tile).astype(jnp.bfloat16)
            partial[span(chunk), :, :, :, columns] = block
            return carry

        lax.fori_loop(0, width // tile, body, 0)

    def back_pair_copy(chunk):
        return pltpu.make_async_remote_copy(
            src_ref=partial.at[span(chunk), other_low],
            dst_ref=pair_in.at[span(chunk)],
            send_sem=back_pair.at[0, chunk],
            recv_sem=back_pair.at[1, chunk],
            device_id=pair_id,
            device_id_type=MESH,
        )

    def back_side_copy(chunk, distance):
        return pltpu.make_async_remote_copy(
            src_ref=pair_sum.at[distance - 1, span(chunk)],
            dst_ref=side_in.at[distance - 1, span(chunk)],
            send_sem=back_side.at[0, chunk, distance - 1],
            recv_sem=back_side.at[1, chunk, distance - 1],
            device_id=side_id(distance),
            device_id_type=MESH,
        )

    def back_copy(step):
        return pltpu.make_async_remote_copy(
            src_ref=served.at[step],
            dst_ref=returned.at[step],
            send_sem=back_send.at[step],
            recv_sem=back_recv.at[step],
            device_id={"sp": lax.rem(me - step + sp_count, sp_count), "tp": tp_me},
            device_id_type=MESH,
        )

    def pair_add(chunk):
        back_pair_copy(chunk).wait_recv()
        for distance in range(1, highs):
            target = side_high(distance)

            def body(index, carry, distance=distance, target=target):
                step = chunk * steps + index
                total = partial[step, low, target].astype(jnp.float32)
                total = total + pair_in[step, target].astype(jnp.float32)
                pair_sum[distance - 1, step] = total.astype(jnp.bfloat16)
                return carry

            lax.fori_loop(0, steps, body, 0)
            back_side_copy(chunk, distance).start()

    def side_add(chunk):
        for distance in range(1, highs):
            back_side_copy(chunk, distance).wait_recv()
        for step in chunk_steps(chunk):
            total = partial[step, low, high].astype(jnp.float32)
            total = total + pair_in[step, high].astype(jnp.float32)
            for distance in range(1, highs):
                total = total + side_in[distance - 1, step].astype(jnp.float32)
            if step == 0:
                returned[0] = total.astype(jnp.bfloat16)
            else:
                served[step] = total.astype(jnp.bfloat16)
                back_copy(step).start()

    for step in range(1, sp_count):
        first_copy(step).start()
    for copy in weight_copies:
        copy.start()

    spread(0)
    for chunk in range(1, chunks - 1):
        spread(chunk)
    pass_on(0)
    settle(0)
    for copy in weight_copies[:2]:
        copy.wait()
    for chunk in range(chunks):
        gate_up(chunk)
        if chunk == 0:
            if chunks > 1:
                spread(chunks - 1)
            weight_copies[2].wait()
        if chunk + 1 < chunks:
            pass_on(chunk + 1)
        if chunk >= 1:
            pair_add(chunk - 1)
        if chunk >= 2:
            side_add(chunk - 2)
        project(chunk)
        back_pair_copy(chunk).start()
        if chunk + 1 < chunks:
            settle(chunk + 1)
    pair_add(chunks - 1)
    if chunks > 1:
        side_add(chunks - 2)
    side_add(chunks - 1)

    for step in range(1, sp_count):
        back_copy(step).wait_recv()
    rows = as_rows(returned[...])
    total = after_ref[...].astype(jnp.float32)
    for pick in range(pick_ref.shape[0]):
        picked = jnp.dot(pick_ref[pick], rows, preferred_element_type=jnp.float32)
        total = total + weight_ref[:, pick : pick + 1] * picked
    out_ref[...] = total.astype(jnp.bfloat16)

    for step in range(sp_count):
        if step > 0:
            first_copy(step).wait_send()
            back_copy(step).wait_send()
        for distance in range(1, highs):
            side_copy(step, distance).wait_send()
        for distance in range(highs):
            pair_copy(step, distance).wait_send()
    for chunk in range(chunks):
        back_pair_copy(chunk).wait_send()
        for distance in range(1, highs):
            back_side_copy(chunk, distance).wait_send()


def routed_experts(send_rows, picks, route_weight, after, w_gate, w_up, w_down):
    sp_count, cap, width = send_rows.shape
    tp_count = lax.axis_size("tp")
    highs = tp_count // LANES
    chunks = 4 if sp_count % 4 == 0 else 1
    chunk_rows = sp_count // chunks * tp_count * cap
    ff_width = w_gate.shape[2]
    half = jnp.bfloat16
    vmem = pl.BlockSpec(memory_space=pltpu.VMEM)
    hbm = pl.BlockSpec(memory_space=pl.ANY)
    dma = pltpu.SemaphoreType.DMA
    return pl.pallas_call(
        functools.partial(expert_kernel, sp_count, tp_count, chunks),
        out_shape=jax.ShapeDtypeStruct(after.shape, half),
        in_specs=[vmem] * 4 + [hbm] * 3,
        out_specs=vmem,
        scratch_shapes=[
            pltpu.VMEM(w_gate.shape[1:], half),
            pltpu.VMEM(w_up.shape[1:], half),
            pltpu.VMEM(w_down.shape[1:], half),
            pltpu.VMEM((sp_count, LANES, highs, cap, width), half),
            pltpu.VMEM((chunk_rows, ff_width), half),
            pltpu.VMEM((sp_count, LANES, highs, cap, width), half),
            pltpu.VMEM((sp_count, highs, cap, width), half),
            pltpu.VMEM((highs - 1, sp_count, cap, width), half),
            pltpu.VMEM((highs - 1, sp_count, cap, width), half),
            pltpu.VMEM((sp_count, cap, width), half),
            pltpu.VMEM((sp_count, cap, width), half),
            dma((4,)),
            dma((sp_count,)),
            dma((sp_count,)),
            dma((sp_count, highs - 1)),
            dma((sp_count, highs - 1)),
            dma((sp_count, highs)),
            dma((sp_count, highs)),
            dma((2, chunks)),
            dma((2, chunks, highs - 1)),
            dma((sp_count,)),
            dma((sp_count,)),
        ],
        compiler_params=pltpu.CompilerParams(
            collective_id=1, has_side_effects=True, vmem_limit_bytes=60 * 1024 * 1024
        ),
    )(send_rows, picks, route_weight, after, w_gate, w_up, w_down)


def per_device(
    stream, mix_gain, pool_weight, pool_scale, ffn_gain, routes, route_weight, w_gate, w_up, w_down
):
    tok_rows, shard_width = stream.shape
    tp_count = lax.axis_size("tp")
    sp_count = lax.axis_size("sp")
    model_width = shard_width * tp_count
    stream_f32 = stream.astype(jnp.float32)
    square = lax.psum(jnp.sum(stream_f32 * stream_f32, axis=1), "tp")
    row_scale = lax.rsqrt(square / model_width + NORM_EPS)[:, None]
    normed = (stream_f32 * row_scale * mix_gain.astype(jnp.float32)).astype(jnp.bfloat16)
    local_groups = pool_weight.shape[0]
    halo_rows = 2 ** (local_groups * tp_count) - 1
    previous = passed_along(normed[tok_rows - halo_rows :], "sp", 1)
    extended = jnp.concatenate([previous, normed], axis=0)
    first_row = lax.axis_index("sp") * tok_rows
    position = first_row + jnp.arange(tok_rows, dtype=jnp.int32)
    source = first_row - halo_rows + jnp.arange(tok_rows + halo_rows, dtype=jnp.int32)
    lag_rows = position[:, None] - source[None, :]
    group_index = lax.axis_index("tp") * local_groups + 0
    window_len = jnp.left_shift(jnp.int32(2), group_index)
    band_mask = ((lag_rows >= 0) & (lag_rows < window_len)).astype(jnp.bfloat16)
    window_sum = jnp.dot(band_mask, extended, preferred_element_type=jnp.float32)
    window_count = jnp.minimum(position + 1, window_len).astype(jnp.float32)[:, None]
    own_rows = normed.astype(jnp.float32)
    pooled = (window_sum / window_count - own_rows).astype(jnp.bfloat16)
    group_outs = jnp.dot(pooled, pool_weight[0], preferred_element_type=jnp.float32)
    mixer_out = group_outs * pool_scale.astype(jnp.float32)
    after_mix = (stream_f32 + mixer_out).astype(jnp.bfloat16)
    token_rows = lax.all_to_all(after_mix, "tp", split_axis=0, concat_axis=1, tiled=True)
    after_f32 = token_rows.astype(jnp.float32)
    ffn_scale = lax.rsqrt(jnp.mean(after_f32 * after_f32, axis=1, keepdims=True) + NORM_EPS)
    normed2 = (after_f32 * ffn_scale * ffn_gain.astype(jnp.float32)).astype(jnp.bfloat16)
    tok_count, top_count = routes.shape
    capacity = 2 * tok_count * top_count // sp_count
    flat_routes = routes.reshape(-1)
    is_expert = (flat_routes[:, None] == jnp.arange(sp_count, dtype=jnp.int32)[None, :]).astype(
        jnp.int32
    )
    slot_rank = jnp.cumsum(is_expert, axis=0) - is_expert
    slot_index = jnp.sum(slot_rank * is_expert, axis=1)
    step_away = lax.rem(flat_routes - lax.axis_index("sp") + sp_count, sp_count)
    dest_slot = (step_away * capacity + slot_index).reshape(tok_count, top_count)
    slot_ids = jnp.arange(sp_count * capacity, dtype=jnp.int32)
    picks = (dest_slot.T[:, :, None] == slot_ids[None, None, :]).astype(jnp.bfloat16)
    dispatch_mask = jnp.sum(picks, axis=0).T
    send_rows = jnp.dot(dispatch_mask, normed2, preferred_element_type=jnp.float32).astype(
        jnp.bfloat16
    )
    send_rows = send_rows.reshape(sp_count, capacity, model_width)
    return routed_experts(send_rows, picks, route_weight, token_rows, w_gate, w_up, w_down)


def solution(mesh):
    in_specs = (
        P("sp", "tp"),
        P("tp"),
        P("tp", None, None),
        P("tp"),
        P(),
        P(("sp", "tp"), None),
        P(("sp", "tp"), None),
        P("sp", None, "tp"),
        P("sp", None, "tp"),
        P("sp", "tp", None),
    )
    out_specs = P(("sp", "tp"), None)
    return jax.shard_map(
        per_device, mesh=mesh, in_specs=in_specs, out_specs=out_specs, check_vma=False
    )
```

```python
import functools

import jax
import jax.numpy as jnp
from jax import lax
from jax.experimental import pallas as pl
from jax.experimental.pallas import tpu as pltpu
from jax.sharding import PartitionSpec as P

NORM_EPS = 1e-06


MESH = pl.DeviceIdType.MESH
COL_TILE = 256
LANES = 2


def as_rows(block):
    width = block.shape[-1]
    if block.shape[-2] % 16:
        return block.astype(jnp.float32).reshape(-1, width).astype(block.dtype)
    return block.reshape(-1, width)


def moves(sp_count):
    far = [(pairs, inner) for pairs in range(1, sp_count // LANES) for inner in range(LANES)]
    return [(0, 0)] + far + [(0, 1)]


def slot_of(expert, me, sp_count):
    pairs = (expert >> 1) - me // LANES
    pairs = jnp.where(pairs < 0, pairs + sp_count // LANES, pairs)
    inner = jnp.where((expert & 1) == lax.rem(me, LANES), 0, 1)
    return jnp.where(pairs == 0, inner * (sp_count - 1), pairs * LANES - 1 + inner)


def as_column(row):
    size = row.shape[1]
    rows = lax.broadcasted_iota(jnp.int32, (size, size), 0)
    columns = lax.broadcasted_iota(jnp.int32, (size, size), 1)
    return jnp.sum(jnp.where(rows == columns, row, 0.0), axis=1, keepdims=True)


def as_row(column):
    size = column.shape[0]
    rows = lax.broadcasted_iota(jnp.int32, (size, size), 0)
    columns = lax.broadcasted_iota(jnp.int32, (size, size), 1)
    return jnp.sum(jnp.where(rows == columns, column, 0.0), axis=0, keepdims=True)


def moved(me, move, sp_count):
    pairs_count = sp_count // LANES
    pairs = lax.rem(me // LANES + move[0], pairs_count)
    return pairs * LANES + lax.rem(me + move[1], LANES)


def moved_back(me, move, sp_count):
    pairs_count = sp_count // LANES
    pairs = lax.rem(me // LANES - move[0] + pairs_count, pairs_count)
    return pairs * LANES + lax.rem(me + move[1], LANES)


def chunk_sizes(sp_count):
    if sp_count % 8:
        return [sp_count]
    return [unit * (sp_count // 8) for unit in (1, 2, 2, 2, 1)]


def col_tile(width):
    return COL_TILE if width % COL_TILE == 0 else width


def expert_kernel(
    sp_count,
    tp_count,
    cap,
    stream_ref,
    mix_ref,
    pool_ref,
    scale_ref,
    gain_ref,
    routes_ref,
    weight_ref,
    gate_hbm,
    up_hbm,
    down_hbm,
    out_ref,
    squares,
    tail,
    halo,
    mixed,
    tokens,
    picked_at,
    send_ref,
    gate,
    up,
    down,
    arrived,
    hidden,
    partial,
    pair_in,
    pair_sum,
    side_in,
    served,
    returned,
    square_sem,
    halo_sem,
    token_sem,
    local_sem,
    first_send,
    first_recv,
    side_send,
    side_recv,
    pair_send,
    pair_recv,
    back_pair,
    back_side,
    back_send,
    back_recv,
):
    me = lax.axis_index("sp")
    tp_me = lax.axis_index("tp")
    high, low = tp_me // LANES, lax.rem(tp_me, LANES)
    highs = tp_count // LANES
    other_low = 1 - low
    pair_id = {"sp": me, "tp": high * LANES + other_low}
    route = moves(sp_count)
    sizes = chunk_sizes(sp_count)
    chunks = len(sizes)
    starts = [sum(sizes[:index]) for index in range(chunks)]
    width = send_ref.shape[2]
    ff_width = gate.shape[1]
    half_width = width // 2

    def side_high(distance):
        return lax.rem(high + distance, highs)

    def side_id(distance):
        return {"sp": me, "tp": side_high(distance) * LANES + low}

    def from_high(distance):
        return lax.rem(high - distance + highs, highs)

    def tp_id(distance):
        return {"sp": me, "tp": lax.rem(tp_me + distance, tp_count)}

    def from_tp(distance):
        return lax.rem(tp_me - distance + tp_count, tp_count)

    weight_copies = [
        pltpu.make_async_copy(source.at[0], target, local_sem.at[index])
        for index, (source, target) in enumerate(((gate_hbm, gate), (up_hbm, up), (down_hbm, down)))
    ]
    own_copy = pltpu.make_async_copy(send_ref.at[0], arrived.at[0, low, high], local_sem.at[3])
    for copy in weight_copies:
        copy.start()

    barrier = pltpu.get_barrier_semaphore()
    for step in range(1, sp_count):
        pl.semaphore_signal(
            barrier,
            inc=1,
            device_id={"sp": moved(me, route[step], sp_count), "tp": tp_me},
            device_id_type=MESH,
        )
    for distance in range(1, tp_count):
        pl.semaphore_signal(barrier, inc=1, device_id=tp_id(distance), device_id_type=MESH)

    def square_copy(distance):
        return pltpu.make_async_remote_copy(
            src_ref=squares.at[0],
            dst_ref=squares.at[distance],
            send_sem=square_sem.at[0, distance - 1],
            recv_sem=square_sem.at[1, distance - 1],
            device_id=tp_id(distance),
            device_id_type=MESH,
        )

    halo_copy = pltpu.make_async_remote_copy(
        src_ref=tail,
        dst_ref=halo,
        send_sem=halo_sem.at[0],
        recv_sem=halo_sem.at[1],
        device_id={"sp": lax.rem(me + 1, sp_count), "tp": tp_me},
        device_id_type=MESH,
    )

    def token_copy(distance):
        return pltpu.make_async_remote_copy(
            src_ref=mixed.at[lax.rem(tp_me + distance, tp_count)],
            dst_ref=tokens.at[tp_me],
            send_sem=token_sem.at[0, distance - 1],
            recv_sem=token_sem.at[1, distance - 1],
            device_id=tp_id(distance),
            device_id_type=MESH,
        )

    tok_rows, group_width = stream_ref.shape
    halo_rows = halo.shape[0]
    tok_count = tokens.shape[1]
    top_count = routes_ref.shape[0]
    slot_count = sp_count * cap
    stream_f32 = stream_ref[...].astype(jnp.float32)
    own_square = as_row(jnp.sum(stream_f32 * stream_f32, axis=1, keepdims=True))
    squares[0] = jnp.broadcast_to(own_square, squares.shape[1:])
    pl.semaphore_wait(barrier, sp_count - 1 + tp_count - 1)
    for distance in range(1, tp_count):
        square_copy(distance).start()

    experts = lax.broadcasted_iota(jnp.int32, (128, tok_count), 0)
    named = [experts == routes_ref[pick : pick + 1, :] for pick in range(top_count)]
    hits = named[0].astype(jnp.float32)
    for pick in range(1, top_count):
        hits = hits + named[pick].astype(jnp.float32)
    earlier = lax.broadcasted_iota(jnp.int32, (tok_count, tok_count), 0)
    later = lax.broadcasted_iota(jnp.int32, (tok_count, tok_count), 1)
    before = jnp.where(earlier < later, 1.0, 0.0).astype(jnp.bfloat16)
    rank = jnp.dot(hits.astype(jnp.bfloat16), before, preferred_element_type=jnp.float32)
    slots = lax.broadcasted_iota(jnp.int32, (slot_count, tok_count), 0).astype(jnp.float32)
    picks = []
    for pick in range(top_count):
        start = slot_of(routes_ref[pick : pick + 1, :], me, sp_count) * cap
        spot = jnp.sum(jnp.where(named[pick], rank, 0.0), axis=0, keepdims=True)
        spot = spot + start.astype(jnp.float32)
        picks.append(jnp.where(slots == spot, 1.0, 0.0))
    dispatch = sum(picks[1:], picks[0]).astype(jnp.bfloat16)
    for pick in range(top_count):
        picked_at[pick] = picks[pick].astype(jnp.bfloat16)

    window_len = jnp.left_shift(jnp.int32(2), tp_me)
    first_row = me * tok_rows
    row_at = lax.broadcasted_iota(jnp.int32, (tok_rows, tok_rows), 0)
    source_at = lax.broadcasted_iota(jnp.int32, (tok_rows, tok_rows), 1)
    lag = row_at - source_at
    band = jnp.where((lag >= 0) & (lag < window_len), 1.0, 0.0).astype(jnp.bfloat16)
    row_at = lax.broadcasted_iota(jnp.int32, (tok_rows, halo_rows), 0)
    source_at = lax.broadcasted_iota(jnp.int32, (tok_rows, halo_rows), 1) - halo_rows
    reach = (row_at - source_at < window_len) & (first_row + source_at >= 0)
    halo_band = jnp.where(reach, 1.0, 0.0).astype(jnp.bfloat16)
    position = first_row + lax.broadcasted_iota(jnp.int32, (tok_rows, 1), 0)
    window_count = jnp.minimum(position + 1, window_len).astype(jnp.float32)

    for distance in range(1, tp_count):
        square_copy(distance).wait_recv()
    square = squares[0, 0:1, :]
    for distance in range(1, tp_count):
        square = square + squares[distance, 0:1, :]
    row_scale = lax.rsqrt(as_column(square) / width + NORM_EPS)
    normed = stream_f32 * row_scale * mix_ref[...].astype(jnp.float32)
    normed = normed.astype(jnp.bfloat16)
    tail[...] = normed[tok_rows - halo_rows :]
    halo_copy.start()
    window_sum = jnp.dot(band, normed, preferred_element_type=jnp.float32)
    halo_copy.wait_recv()
    window_sum = window_sum + jnp.dot(halo_band, halo[...], preferred_element_type=jnp.float32)
    pooled = (window_sum / window_count - normed.astype(jnp.float32)).astype(jnp.bfloat16)
    mixer_out = jnp.dot(pooled, pool_ref[0], preferred_element_type=jnp.float32)
    mixer_out = mixer_out * scale_ref[...].astype(jnp.float32)
    after_mix = (stream_f32 + mixer_out).astype(jnp.bfloat16)
    mixed[...] = after_mix.reshape(mixed.shape)
    for distance in range(1, tp_count):
        token_copy(distance).start()
    tokens[tp_me] = mixed[tp_me]
    for distance in range(1, tp_count):
        token_copy(distance).wait_recv()
    mean_square = jnp.zeros((tok_count, 1), jnp.float32)
    for piece in range(tp_count):
        after_f32 = tokens[piece].astype(jnp.float32)
        mean_square = mean_square + jnp.sum(after_f32 * after_f32, axis=1, keepdims=True)
    ffn_scale = lax.rsqrt(mean_square / width + NORM_EPS)
    for piece in range(tp_count):
        columns = slice(piece * group_width, (piece + 1) * group_width)
        gain = gain_ref[:, columns].astype(jnp.float32)
        normed2 = (tokens[piece].astype(jnp.float32) * ffn_scale * gain).astype(jnp.bfloat16)
        rows = jnp.dot(dispatch, normed2, preferred_element_type=jnp.float32)
        rows = rows.reshape(sp_count, cap, group_width).astype(jnp.bfloat16)
        send_ref[:, :, columns] = rows

    def first_copy(step):
        return pltpu.make_async_remote_copy(
            src_ref=send_ref.at[step],
            dst_ref=arrived.at[step, low, high],
            send_sem=first_send.at[step],
            recv_sem=first_recv.at[step],
            device_id={"sp": moved(me, route[step], sp_count), "tp": tp_me},
            device_id_type=MESH,
        )

    def side_copy(step, distance):
        return pltpu.make_async_remote_copy(
            src_ref=arrived.at[step, low, high],
            dst_ref=arrived.at[step, low, high],
            send_sem=side_send.at[step, distance - 1],
            recv_sem=side_recv.at[step, distance - 1],
            device_id=side_id(distance),
            device_id_type=MESH,
        )

    def pair_copy(step, distance):
        block = arrived.at[step, low, from_high(distance)]
        return pltpu.make_async_remote_copy(
            src_ref=block,
            dst_ref=block,
            send_sem=pair_send.at[step, distance],
            recv_sem=pair_recv.at[step, distance],
            device_id=pair_id,
            device_id_type=MESH,
        )

    def chunk_steps(chunk):
        return range(starts[chunk], starts[chunk] + sizes[chunk])

    def spread(chunk):
        for step in chunk_steps(chunk):
            if step == 0:
                own_copy.wait()
            else:
                first_copy(step).wait_recv()
            for distance in range(1, highs):
                side_copy(step, distance).start()
            pair_copy(step, 0).start()

    def pass_on(chunk):
        for step in chunk_steps(chunk):
            for distance in range(1, highs):
                side_copy(step, distance).wait_recv()
                pair_copy(step, distance).start()

    def settle(chunk):
        for step in chunk_steps(chunk):
            for distance in range(highs):
                pair_copy(step, distance).wait_recv()

    def span(chunk):
        return pl.ds(starts[chunk], sizes[chunk])

    def row_span(chunk):
        return pl.ds(0, sizes[chunk] * tp_count * cap)

    def gate_up(chunk, first, last):
        tile = col_tile(ff_width)

        def body(index, carry):
            columns = pl.ds(pl.multiple_of(index * tile, tile), tile)
            rows = as_rows(arrived[span(chunk)])
            gate_val = jnp.dot(rows, gate[:, columns], preferred_element_type=jnp.float32)
            up_val = jnp.dot(rows, up[:, columns], preferred_element_type=jnp.float32)
            hidden[row_span(chunk), columns] = (jax.nn.silu(gate_val) * up_val).astype(jnp.bfloat16)
            return carry

        lax.fori_loop(first, last, body, 0)

    def project(chunk, half):
        tile = col_tile(half_width)
        first = half * half_width // tile

        def body(index, carry):
            columns = pl.ds(pl.multiple_of(index * tile, tile), tile)
            block = jnp.dot(
                hidden[row_span(chunk), :], down[:, columns], preferred_element_type=jnp.float32
            )
            block = block.reshape(sizes[chunk], LANES, highs, cap, tile).astype(jnp.bfloat16)
            partial[span(chunk), :, :, :, columns] = block
            return carry

        lax.fori_loop(first, first + half_width // tile, body, 0)

    def part(half):
        return pl.ds(half * half_width, half_width)

    def back_pair_copy(chunk, half):
        return pltpu.make_async_remote_copy(
            src_ref=partial.at[span(chunk), other_low, :, :, part(half)],
            dst_ref=pair_in.at[span(chunk), :, :, part(half)],
            send_sem=back_pair.at[0, chunk, half],
            recv_sem=back_pair.at[1, chunk, half],
            device_id=pair_id,
            device_id_type=MESH,
        )

    def back_side_copy(chunk, half, distance):
        return pltpu.make_async_remote_copy(
            src_ref=pair_sum.at[distance - 1, span(chunk), :, part(half)],
            dst_ref=side_in.at[distance - 1, span(chunk), :, part(half)],
            send_sem=back_side.at[0, chunk, half, distance - 1],
            recv_sem=back_side.at[1, chunk, half, distance - 1],
            device_id=side_id(distance),
            device_id_type=MESH,
        )

    def back_copy(step, half):
        return pltpu.make_async_remote_copy(
            src_ref=served.at[step, :, part(half)],
            dst_ref=returned.at[step, :, part(half)],
            send_sem=back_send.at[step, half],
            recv_sem=back_recv.at[step, half],
            device_id={"sp": moved_back(me, route[step], sp_count), "tp": tp_me},
            device_id_type=MESH,
        )

    def pair_add(chunk, half):
        back_pair_copy(chunk, half).wait_recv()
        for distance in range(1, highs):
            target = side_high(distance)

            def body(index, carry, distance=distance, target=target):
                step = starts[chunk] + index
                total = partial[step, low, target, :, part(half)].astype(jnp.float32)
                total = total + pair_in[step, target, :, part(half)].astype(jnp.float32)
                pair_sum[distance - 1, step, :, part(half)] = total.astype(jnp.bfloat16)
                return carry

            lax.fori_loop(0, sizes[chunk], body, 0)
            back_side_copy(chunk, half, distance).start()

    def side_add(chunk, half):
        for distance in range(1, highs):
            back_side_copy(chunk, half, distance).wait_recv()
        for step in chunk_steps(chunk):
            total = partial[step, low, high, :, part(half)].astype(jnp.float32)
            total = total + pair_in[step, high, :, part(half)].astype(jnp.float32)
            for distance in range(1, highs):
                total = total + side_in[distance - 1, step, :, part(half)].astype(jnp.float32)
            if step == 0:
                returned[0, :, part(half)] = total.astype(jnp.bfloat16)
            else:
                served[step, :, part(half)] = total.astype(jnp.bfloat16)
                back_copy(step, half).start()

    own_copy.start()
    for step in range(1, sp_count):
        first_copy(step).start()

    last = chunks - 1
    spread(0)
    pass_on(0)
    if chunks > 1:
        spread(last)
    settle(0)
    for copy in weight_copies:
        copy.wait()
    tiles = ff_width // col_tile(ff_width)
    early, late = tiles // 2, tiles - tiles // 4
    for chunk in range(chunks):
        gate_up(chunk, 0, early)
        if chunk == 0 and chunks > 1:
            pass_on(last)
            spread(1)
        if chunk >= 1:
            pair_add(chunk - 1, 0)
            pair_add(chunk - 1, 1)
        gate_up(chunk, early, late)
        if chunk >= 2:
            side_add(chunk - 2, 0)
            side_add(chunk - 2, 1)
        gate_up(chunk, late, tiles)
        if chunk == 1:
            spread(2)
        if chunk == 2:
            pass_on(3)
        for half in range(2):
            project(chunk, half)
            back_pair_copy(chunk, half).start()
        if chunk < 2 and chunks > 1:
            pass_on(chunk + 1)
        if chunk < last:
            settle(chunk + 1)
        if chunk == 1:
            spread(3)
    pair_add(last, 0)
    pair_add(last, 1)
    for half in range(2):
        if chunks > 1:
            side_add(last - 1, half)
    for half in range(2):
        side_add(last, half)

    for step in range(1, sp_count):
        for half in range(2):
            back_copy(step, half).wait_recv()
    rows = as_rows(returned[...])
    route_weights = [as_column(weight_ref[pick : pick + 1, :]) for pick in range(top_count)]
    for piece in range(tp_count):
        columns = slice(piece * group_width, (piece + 1) * group_width)
        total = tokens[piece].astype(jnp.float32)
        for pick in range(top_count):
            picked = lax.dot_general(
                picked_at[pick],
                rows[:, columns],
                (((0,), (0,)), ((), ())),
                preferred_element_type=jnp.float32,
            )
            total = total + route_weights[pick] * picked
        out_ref[:, columns] = total.astype(jnp.bfloat16)

    halo_copy.wait_send()
    for distance in range(1, tp_count):
        square_copy(distance).wait_send()
        token_copy(distance).wait_send()
    for step in range(sp_count):
        if step > 0:
            first_copy(step).wait_send()
            for half in range(2):
                back_copy(step, half).wait_send()
        for distance in range(1, highs):
            side_copy(step, distance).wait_send()
        for distance in range(highs):
            pair_copy(step, distance).wait_send()
    for chunk in range(chunks):
        for half in range(2):
            back_pair_copy(chunk, half).wait_send()
            for distance in range(1, highs):
                back_side_copy(chunk, half, distance).wait_send()


def per_device(
    stream, mix_gain, pool_weight, pool_scale, ffn_gain, routes, route_weight, w_gate, w_up, w_down
):
    tok_rows, group_width = stream.shape
    tp_count = lax.axis_size("tp")
    sp_count = lax.axis_size("sp")
    width = group_width * tp_count
    tok_count, top_count = routes.shape
    cap = 2 * tok_count * top_count // sp_count
    halo_rows = 2 ** (pool_weight.shape[0] * tp_count)
    highs = tp_count // LANES
    chunks = len(chunk_sizes(sp_count))
    chunk_rows = max(chunk_sizes(sp_count)) * tp_count * cap
    ff_width = w_gate.shape[2]
    half = jnp.bfloat16
    vmem = pl.BlockSpec(memory_space=pltpu.VMEM)
    hbm = pl.BlockSpec(memory_space=pl.ANY)
    dma = pltpu.SemaphoreType.DMA
    return pl.pallas_call(
        functools.partial(expert_kernel, sp_count, tp_count, cap),
        out_shape=jax.ShapeDtypeStruct((tok_count, width), half),
        in_specs=[vmem] * 7 + [hbm] * 3,
        out_specs=vmem,
        scratch_shapes=[
            pltpu.VMEM((tp_count, 8, tok_rows), jnp.float32),
            pltpu.VMEM((halo_rows, group_width), half),
            pltpu.VMEM((halo_rows, group_width), half),
            pltpu.VMEM((tp_count, tok_count, group_width), half),
            pltpu.VMEM((tp_count, tok_count, group_width), half),
            pltpu.VMEM((top_count, sp_count * cap, tok_count), half),
            pltpu.VMEM((sp_count, cap, width), half),
            pltpu.VMEM(w_gate.shape[1:], half),
            pltpu.VMEM(w_up.shape[1:], half),
            pltpu.VMEM(w_down.shape[1:], half),
            pltpu.VMEM((sp_count, LANES, highs, cap, width), half),
            pltpu.VMEM((chunk_rows, ff_width), half),
            pltpu.VMEM((sp_count, LANES, highs, cap, width), half),
            pltpu.VMEM((sp_count, highs, cap, width), half),
            pltpu.VMEM((highs - 1, sp_count, cap, width), half),
            pltpu.VMEM((highs - 1, sp_count, cap, width), half),
            pltpu.VMEM((sp_count, cap, width), half),
            pltpu.VMEM((sp_count, cap, width), half),
            dma((2, tp_count - 1)),
            dma((2,)),
            dma((2, tp_count - 1)),
            dma((4,)),
            dma((sp_count,)),
            dma((sp_count,)),
            dma((sp_count, highs - 1)),
            dma((sp_count, highs - 1)),
            dma((sp_count, highs)),
            dma((sp_count, highs)),
            dma((2, chunks, 2)),
            dma((2, chunks, 2, highs - 1)),
            dma((sp_count, 2)),
            dma((sp_count, 2)),
        ],
        compiler_params=pltpu.CompilerParams(
            collective_id=1, has_side_effects=True, vmem_limit_bytes=60 * 1024 * 1024
        ),
    )(
        stream,
        mix_gain[None, :],
        pool_weight,
        pool_scale[None, :],
        ffn_gain[None, :],
        routes.T,
        route_weight.T,
        w_gate,
        w_up,
        w_down,
    )


def solution(mesh):
    in_specs = (
        P("sp", "tp"),
        P("tp"),
        P("tp", None, None),
        P("tp"),
        P(),
        P(("sp", "tp"), None),
        P(("sp", "tp"), None),
        P("sp", None, "tp"),
        P("sp", None, "tp"),
        P("sp", "tp", None),
    )
    out_specs = P(("sp", "tp"), None)
    return jax.shard_map(
        per_device, mesh=mesh, in_specs=in_specs, out_specs=out_specs, check_vma=False
    )
```

```python
import functools

import jax
import jax.numpy as jnp
from jax import lax
from jax.experimental import pallas as pl
from jax.experimental.pallas import tpu as pltpu
from jax.sharding import PartitionSpec as P

NORM_EPS = 1e-06


MESH = pl.DeviceIdType.MESH
COL_TILE = 256
LANES = 2
CHUNK_UNITS = (2, 2, 2, 1, 1)
PLAN = {
    "pre": "s0 p0 s1 e0",
    "0l": "p1 s2",
    "0z": "e1",
    "1e": "a0 s3",
    "1l": "p2 s4",
    "1z": "e2",
    "2e": "a1 b0",
    "2l": "p3 p4",
    "2z": "e3",
    "3e": "a2 b1",
    "3z": "e4",
    "4e": "a3 b2",
    "post": "a4 b3 b4",
}
SINGLE_PLAN = {"pre": "s0 p0 e0", "post": "a0 b0"}


def as_rows(block):
    width = block.shape[-1]
    if block.shape[-2] % 16:
        return block.astype(jnp.float32).reshape(-1, width).astype(block.dtype)
    return block.reshape(-1, width)


def moves(sp_count):
    far = [(pairs, inner) for pairs in range(1, sp_count // LANES) for inner in range(LANES)]
    return [(0, 0), (0, 1)] + far


def slot_of(expert, me, sp_count):
    pairs = (expert >> 1) - me // LANES
    pairs = jnp.where(pairs < 0, pairs + sp_count // LANES, pairs)
    inner = jnp.where((expert & 1) == lax.rem(me, LANES), 0, 1)
    return pairs * LANES + inner


def as_column(row):
    size = row.shape[1]
    rows = lax.broadcasted_iota(jnp.int32, (size, size), 0)
    columns = lax.broadcasted_iota(jnp.int32, (size, size), 1)
    return jnp.sum(jnp.where(rows == columns, row, 0.0), axis=1, keepdims=True)


def as_row(column):
    size = column.shape[0]
    rows = lax.broadcasted_iota(jnp.int32, (size, size), 0)
    columns = lax.broadcasted_iota(jnp.int32, (size, size), 1)
    return jnp.sum(jnp.where(rows == columns, column, 0.0), axis=0, keepdims=True)


def moved(me, move, sp_count):
    pairs_count = sp_count // LANES
    pairs = lax.rem(me // LANES + move[0], pairs_count)
    return pairs * LANES + lax.rem(me + move[1], LANES)


def moved_back(me, move, sp_count):
    pairs_count = sp_count // LANES
    pairs = lax.rem(me // LANES - move[0] + pairs_count, pairs_count)
    return pairs * LANES + lax.rem(me + move[1], LANES)


def chunk_sizes(sp_count):
    if sp_count % 8:
        return [sp_count]
    return [unit * (sp_count // 8) for unit in CHUNK_UNITS]


def col_tile(width):
    return COL_TILE if width % COL_TILE == 0 else width


def expert_kernel(
    sp_count,
    tp_count,
    cap,
    stream_ref,
    mix_ref,
    pool_ref,
    scale_ref,
    gain_ref,
    routes_ref,
    weight_ref,
    gate_hbm,
    up_hbm,
    down_hbm,
    out_ref,
    squares,
    tail,
    halo,
    mixed,
    tokens,
    picked_at,
    send_ref,
    gate,
    up,
    down,
    arrived,
    hidden,
    partial,
    pair_in,
    pair_sum,
    side_in,
    served,
    returned,
    square_sem,
    halo_sem,
    token_sem,
    local_sem,
    first_send,
    first_recv,
    side_send,
    side_recv,
    pair_send,
    pair_recv,
    back_pair,
    back_side,
    back_send,
    back_recv,
):
    me = lax.axis_index("sp")
    tp_me = lax.axis_index("tp")
    high, low = tp_me // LANES, lax.rem(tp_me, LANES)
    highs = tp_count // LANES
    other_low = 1 - low
    pair_id = {"sp": me, "tp": high * LANES + other_low}
    route = moves(sp_count)
    sizes = chunk_sizes(sp_count)
    chunks = len(sizes)
    starts = [sum(sizes[:index]) for index in range(chunks)]
    width = send_ref.shape[2]
    ff_width = gate.shape[1]
    half_width = width // 2

    def side_high(distance):
        return lax.rem(high + distance, highs)

    def side_id(distance):
        return {"sp": me, "tp": side_high(distance) * LANES + low}

    def from_high(distance):
        return lax.rem(high - distance + highs, highs)

    def tp_id(distance):
        return {"sp": me, "tp": lax.rem(tp_me + distance, tp_count)}

    def from_tp(distance):
        return lax.rem(tp_me - distance + tp_count, tp_count)

    weight_copies = [
        pltpu.make_async_copy(source.at[0], target, local_sem.at[index])
        for index, (source, target) in enumerate(((gate_hbm, gate), (up_hbm, up), (down_hbm, down)))
    ]
    own_copy = pltpu.make_async_copy(send_ref.at[0], arrived.at[0, low, high], local_sem.at[3])
    for copy in weight_copies:
        copy.start()

    barrier = pltpu.get_barrier_semaphore()
    for step in range(1, sp_count):
        pl.semaphore_signal(
            barrier,
            inc=1,
            device_id={"sp": moved(me, route[step], sp_count), "tp": tp_me},
            device_id_type=MESH,
        )
    for distance in range(1, tp_count):
        pl.semaphore_signal(barrier, inc=1, device_id=tp_id(distance), device_id_type=MESH)

    def square_copy(distance):
        return pltpu.make_async_remote_copy(
            src_ref=squares.at[0],
            dst_ref=squares.at[distance],
            send_sem=square_sem.at[0, distance - 1],
            recv_sem=square_sem.at[1, distance - 1],
            device_id=tp_id(distance),
            device_id_type=MESH,
        )

    halo_copy = pltpu.make_async_remote_copy(
        src_ref=tail,
        dst_ref=halo,
        send_sem=halo_sem.at[0],
        recv_sem=halo_sem.at[1],
        device_id={"sp": lax.rem(me + 1, sp_count), "tp": tp_me},
        device_id_type=MESH,
    )

    def token_copy(distance):
        return pltpu.make_async_remote_copy(
            src_ref=mixed.at[lax.rem(tp_me + distance, tp_count)],
            dst_ref=tokens.at[tp_me],
            send_sem=token_sem.at[0, distance - 1],
            recv_sem=token_sem.at[1, distance - 1],
            device_id=tp_id(distance),
            device_id_type=MESH,
        )

    tok_rows, group_width = stream_ref.shape
    halo_rows = halo.shape[0]
    tok_count = tokens.shape[1]
    top_count = routes_ref.shape[0]
    slot_count = sp_count * cap
    stream_f32 = stream_ref[...].astype(jnp.float32)
    own_square = as_row(jnp.sum(stream_f32 * stream_f32, axis=1, keepdims=True))
    squares[0] = jnp.broadcast_to(own_square, squares.shape[1:])
    pl.semaphore_wait(barrier, sp_count - 1 + tp_count - 1)
    for distance in range(1, tp_count):
        square_copy(distance).start()

    experts = lax.broadcasted_iota(jnp.int32, (128, tok_count), 0)
    named = [experts == routes_ref[pick : pick + 1, :] for pick in range(top_count)]
    hits = named[0].astype(jnp.float32)
    for pick in range(1, top_count):
        hits = hits + named[pick].astype(jnp.float32)
    earlier = lax.broadcasted_iota(jnp.int32, (tok_count, tok_count), 0)
    later = lax.broadcasted_iota(jnp.int32, (tok_count, tok_count), 1)
    before = jnp.where(earlier < later, 1.0, 0.0).astype(jnp.bfloat16)
    rank = jnp.dot(hits.astype(jnp.bfloat16), before, preferred_element_type=jnp.float32)
    slots = lax.broadcasted_iota(jnp.int32, (slot_count, tok_count), 0).astype(jnp.float32)
    picks = []
    for pick in range(top_count):
        start = slot_of(routes_ref[pick : pick + 1, :], me, sp_count) * cap
        spot = jnp.sum(jnp.where(named[pick], rank, 0.0), axis=0, keepdims=True)
        spot = spot + start.astype(jnp.float32)
        picks.append(jnp.where(slots == spot, 1.0, 0.0))
    dispatch = sum(picks[1:], picks[0]).astype(jnp.bfloat16)
    for pick in range(top_count):
        picked_at[pick] = picks[pick].astype(jnp.bfloat16)

    window_len = jnp.left_shift(jnp.int32(2), tp_me)
    first_row = me * tok_rows
    row_at = lax.broadcasted_iota(jnp.int32, (tok_rows, tok_rows), 0)
    source_at = lax.broadcasted_iota(jnp.int32, (tok_rows, tok_rows), 1)
    lag = row_at - source_at
    band = jnp.where((lag >= 0) & (lag < window_len), 1.0, 0.0).astype(jnp.bfloat16)
    row_at = lax.broadcasted_iota(jnp.int32, (tok_rows, halo_rows), 0)
    source_at = lax.broadcasted_iota(jnp.int32, (tok_rows, halo_rows), 1) - halo_rows
    reach = (row_at - source_at < window_len) & (first_row + source_at >= 0)
    halo_band = jnp.where(reach, 1.0, 0.0).astype(jnp.bfloat16)
    position = first_row + lax.broadcasted_iota(jnp.int32, (tok_rows, 1), 0)
    window_count = jnp.minimum(position + 1, window_len).astype(jnp.float32)

    for distance in range(1, tp_count):
        square_copy(distance).wait_recv()
    square = squares[0, 0:1, :]
    for distance in range(1, tp_count):
        square = square + squares[distance, 0:1, :]
    row_scale = lax.rsqrt(as_column(square) / width + NORM_EPS)
    normed = stream_f32 * row_scale * mix_ref[...].astype(jnp.float32)[None, :]
    normed = normed.astype(jnp.bfloat16)
    tail[...] = normed[tok_rows - halo_rows :]
    halo_copy.start()
    window_sum = jnp.dot(band, normed, preferred_element_type=jnp.float32)
    halo_copy.wait_recv()
    window_sum = window_sum + jnp.dot(halo_band, halo[...], preferred_element_type=jnp.float32)
    pooled = (window_sum / window_count - normed.astype(jnp.float32)).astype(jnp.bfloat16)
    mixer_out = jnp.dot(pooled, pool_ref[0], preferred_element_type=jnp.float32)
    mixer_out = mixer_out * scale_ref[...].astype(jnp.float32)[None, :]
    after_mix = (stream_f32 + mixer_out).astype(jnp.bfloat16)
    mixed[...] = after_mix.reshape(mixed.shape)
    for distance in range(1, tp_count):
        token_copy(distance).start()
    tokens[tp_me] = mixed[tp_me]
    for distance in range(1, tp_count):
        token_copy(distance).wait_recv()
    mean_square = jnp.zeros((tok_count, 1), jnp.float32)
    for piece in range(tp_count):
        after_f32 = tokens[piece].astype(jnp.float32)
        mean_square = mean_square + jnp.sum(after_f32 * after_f32, axis=1, keepdims=True)
    ffn_scale = lax.rsqrt(mean_square / width + NORM_EPS)
    for piece in range(tp_count):
        columns = slice(piece * group_width, (piece + 1) * group_width)
        gain = gain_ref[columns].astype(jnp.float32)[None, :]
        normed2 = (tokens[piece].astype(jnp.float32) * ffn_scale * gain).astype(jnp.bfloat16)
        rows = jnp.dot(dispatch, normed2, preferred_element_type=jnp.float32)
        rows = rows.reshape(sp_count, cap, group_width).astype(jnp.bfloat16)
        send_ref[:, :, columns] = rows

    def first_copy(step):
        return pltpu.make_async_remote_copy(
            src_ref=send_ref.at[step],
            dst_ref=arrived.at[step, low, high],
            send_sem=first_send.at[step],
            recv_sem=first_recv.at[step],
            device_id={"sp": moved(me, route[step], sp_count), "tp": tp_me},
            device_id_type=MESH,
        )

    def side_copy(step, distance):
        return pltpu.make_async_remote_copy(
            src_ref=arrived.at[step, low, high],
            dst_ref=arrived.at[step, low, high],
            send_sem=side_send.at[step, distance - 1],
            recv_sem=side_recv.at[step, distance - 1],
            device_id=side_id(distance),
            device_id_type=MESH,
        )

    def pair_copy(step, distance):
        block = arrived.at[step, low, from_high(distance)]
        return pltpu.make_async_remote_copy(
            src_ref=block,
            dst_ref=block,
            send_sem=pair_send.at[step, distance],
            recv_sem=pair_recv.at[step, distance],
            device_id=pair_id,
            device_id_type=MESH,
        )

    def chunk_steps(chunk):
        return range(starts[chunk], starts[chunk] + sizes[chunk])

    def spread(chunk):
        for step in chunk_steps(chunk):
            if step == 0:
                own_copy.wait()
            else:
                first_copy(step).wait_recv()
            for distance in range(1, highs):
                side_copy(step, distance).start()
            pair_copy(step, 0).start()

    def pass_on(chunk):
        for step in chunk_steps(chunk):
            for distance in range(1, highs):
                side_copy(step, distance).wait_recv()
                pair_copy(step, distance).start()

    def settle(chunk):
        for step in chunk_steps(chunk):
            for distance in range(highs):
                pair_copy(step, distance).wait_recv()

    def span(chunk):
        return pl.ds(starts[chunk], sizes[chunk])

    def row_span(chunk):
        return pl.ds(0, sizes[chunk] * tp_count * cap)

    def gate_up(chunk, first, last):
        tile = col_tile(ff_width)

        def body(index, carry):
            columns = pl.ds(pl.multiple_of(index * tile, tile), tile)
            rows = as_rows(arrived[span(chunk)])
            gate_val = jnp.dot(rows, gate[:, columns], preferred_element_type=jnp.float32)
            up_val = jnp.dot(rows, up[:, columns], preferred_element_type=jnp.float32)
            hidden[row_span(chunk), columns] = (jax.nn.silu(gate_val) * up_val).astype(jnp.bfloat16)
            return carry

        lax.fori_loop(first, last, body, 0)

    def project(chunk, half):
        tile = col_tile(half_width)
        first = half * half_width // tile

        def body(index, carry):
            columns = pl.ds(pl.multiple_of(index * tile, tile), tile)
            block = jnp.dot(
                hidden[row_span(chunk), :], down[:, columns], preferred_element_type=jnp.float32
            )
            block = block.reshape(sizes[chunk], LANES, highs, cap, tile).astype(jnp.bfloat16)
            partial[span(chunk), :, :, :, columns] = block
            return carry

        lax.fori_loop(first, first + half_width // tile, body, 0)

    def part(half):
        return pl.ds(half * half_width, half_width)

    def back_pair_copy(chunk, half):
        return pltpu.make_async_remote_copy(
            src_ref=partial.at[span(chunk), other_low, :, :, part(half)],
            dst_ref=pair_in.at[span(chunk), :, :, part(half)],
            send_sem=back_pair.at[0, chunk, half],
            recv_sem=back_pair.at[1, chunk, half],
            device_id=pair_id,
            device_id_type=MESH,
        )

    def back_side_copy(chunk, half, distance):
        return pltpu.make_async_remote_copy(
            src_ref=pair_sum.at[distance - 1, span(chunk), :, part(half)],
            dst_ref=side_in.at[distance - 1, span(chunk), :, part(half)],
            send_sem=back_side.at[0, chunk, half, distance - 1],
            recv_sem=back_side.at[1, chunk, half, distance - 1],
            device_id=side_id(distance),
            device_id_type=MESH,
        )

    def back_copy(step, half):
        return pltpu.make_async_remote_copy(
            src_ref=served.at[step, :, part(half)],
            dst_ref=returned.at[step, :, part(half)],
            send_sem=back_send.at[step, half],
            recv_sem=back_recv.at[step, half],
            device_id={"sp": moved_back(me, route[step], sp_count), "tp": tp_me},
            device_id_type=MESH,
        )

    def pair_add(chunk, half):
        back_pair_copy(chunk, half).wait_recv()
        for distance in range(1, highs):
            target = side_high(distance)

            def body(index, carry, distance=distance, target=target):
                step = starts[chunk] + index
                total = partial[step, low, target, :, part(half)].astype(jnp.float32)
                total = total + pair_in[step, target, :, part(half)].astype(jnp.float32)
                pair_sum[distance - 1, step, :, part(half)] = total.astype(jnp.bfloat16)
                return carry

            lax.fori_loop(0, sizes[chunk], body, 0)
            back_side_copy(chunk, half, distance).start()

    def side_add(chunk, half):
        for distance in range(1, highs):
            back_side_copy(chunk, half, distance).wait_recv()
        for step in chunk_steps(chunk):
            total = partial[step, low, high, :, part(half)].astype(jnp.float32)
            total = total + pair_in[step, high, :, part(half)].astype(jnp.float32)
            for distance in range(1, highs):
                total = total + side_in[distance - 1, step, :, part(half)].astype(jnp.float32)
            if step == 0:
                returned[0, :, part(half)] = total.astype(jnp.bfloat16)
            else:
                served[step, :, part(half)] = total.astype(jnp.bfloat16)
                back_copy(step, half).start()

    own_copy.start()
    for step in range(1, sp_count):
        first_copy(step).start()

    plan = PLAN if chunks == len(CHUNK_UNITS) else SINGLE_PLAN
    acts = {"s": spread, "p": pass_on, "e": settle}
    adds = {"a": pair_add, "b": side_add}

    def run(place):
        for name in plan.get(place, "").split():
            if name[0] in acts:
                acts[name[0]](int(name[1]))
            elif len(name) > 2:
                adds[name[0]](int(name[1]), int(name[2]))
            else:
                for half in range(2):
                    adds[name[0]](int(name[1]), half)

    run("pre")
    for copy in weight_copies:
        copy.wait()
    tiles = ff_width // col_tile(ff_width)
    early, late = tiles // 2, tiles - tiles // 4
    for chunk in range(chunks):
        gate_up(chunk, 0, early)
        run(f"{chunk}e")
        gate_up(chunk, early, late)
        run(f"{chunk}m")
        gate_up(chunk, late, tiles)
        run(f"{chunk}l")
        for half in range(2):
            project(chunk, half)
            back_pair_copy(chunk, half).start()
            run(f"{chunk}h" if half == 0 else f"{chunk}z")
    run("post")

    for step in range(1, sp_count):
        for half in range(2):
            back_copy(step, half).wait_recv()
    rows = as_rows(returned[...])
    route_weights = [as_column(weight_ref[pick : pick + 1, :]) for pick in range(top_count)]
    for piece in range(tp_count):
        columns = slice(piece * group_width, (piece + 1) * group_width)
        total = tokens[piece].astype(jnp.float32)
        for pick in range(top_count):
            picked = lax.dot_general(
                picked_at[pick],
                rows[:, columns],
                (((0,), (0,)), ((), ())),
                preferred_element_type=jnp.float32,
            )
            total = total + route_weights[pick] * picked
        out_ref[:, columns] = total.astype(jnp.bfloat16)

    halo_copy.wait_send()
    for distance in range(1, tp_count):
        square_copy(distance).wait_send()
        token_copy(distance).wait_send()
    for step in range(sp_count):
        if step > 0:
            first_copy(step).wait_send()
            for half in range(2):
                back_copy(step, half).wait_send()
        for distance in range(1, highs):
            side_copy(step, distance).wait_send()
        for distance in range(highs):
            pair_copy(step, distance).wait_send()
    for chunk in range(chunks):
        for half in range(2):
            back_pair_copy(chunk, half).wait_send()
            for distance in range(1, highs):
                back_side_copy(chunk, half, distance).wait_send()


def per_device(
    stream, mix_gain, pool_weight, pool_scale, ffn_gain, routes, route_weight, w_gate, w_up, w_down
):
    tok_rows, group_width = stream.shape
    tp_count = lax.axis_size("tp")
    sp_count = lax.axis_size("sp")
    width = group_width * tp_count
    tok_count, top_count = routes.shape
    cap = 2 * tok_count * top_count // sp_count
    halo_rows = 2 ** (pool_weight.shape[0] * tp_count)
    highs = tp_count // LANES
    chunks = len(chunk_sizes(sp_count))
    chunk_rows = max(chunk_sizes(sp_count)) * tp_count * cap
    ff_width = w_gate.shape[2]
    half = jnp.bfloat16
    vmem = pl.BlockSpec(memory_space=pltpu.VMEM)
    hbm = pl.BlockSpec(memory_space=pl.ANY)
    dma = pltpu.SemaphoreType.DMA
    return pl.pallas_call(
        functools.partial(expert_kernel, sp_count, tp_count, cap),
        out_shape=jax.ShapeDtypeStruct((tok_count, width), half),
        in_specs=[vmem] * 7 + [hbm] * 3,
        out_specs=vmem,
        scratch_shapes=[
            pltpu.VMEM((tp_count, 8, tok_rows), jnp.float32),
            pltpu.VMEM((halo_rows, group_width), half),
            pltpu.VMEM((halo_rows, group_width), half),
            pltpu.VMEM((tp_count, tok_count, group_width), half),
            pltpu.VMEM((tp_count, tok_count, group_width), half),
            pltpu.VMEM((top_count, sp_count * cap, tok_count), half),
            pltpu.VMEM((sp_count, cap, width), half),
            pltpu.VMEM(w_gate.shape[1:], half),
            pltpu.VMEM(w_up.shape[1:], half),
            pltpu.VMEM(w_down.shape[1:], half),
            pltpu.VMEM((sp_count, LANES, highs, cap, width), half),
            pltpu.VMEM((chunk_rows, ff_width), half),
            pltpu.VMEM((sp_count, LANES, highs, cap, width), half),
            pltpu.VMEM((sp_count, highs, cap, width), half),
            pltpu.VMEM((highs - 1, sp_count, cap, width), half),
            pltpu.VMEM((highs - 1, sp_count, cap, width), half),
            pltpu.VMEM((sp_count, cap, width), half),
            pltpu.VMEM((sp_count, cap, width), half),
            dma((2, tp_count - 1)),
            dma((2,)),
            dma((2, tp_count - 1)),
            dma((4,)),
            dma((sp_count,)),
            dma((sp_count,)),
            dma((sp_count, highs - 1)),
            dma((sp_count, highs - 1)),
            dma((sp_count, highs)),
            dma((sp_count, highs)),
            dma((2, chunks, 2)),
            dma((2, chunks, 2, highs - 1)),
            dma((sp_count, 2)),
            dma((sp_count, 2)),
        ],
        compiler_params=pltpu.CompilerParams(
            collective_id=1, has_side_effects=True, vmem_limit_bytes=60 * 1024 * 1024
        ),
    )(
        stream,
        mix_gain,
        pool_weight,
        pool_scale,
        ffn_gain,
        routes.T,
        route_weight.T,
        w_gate,
        w_up,
        w_down,
    )


def solution(mesh):
    in_specs = (
        P("sp", "tp"),
        P("tp"),
        P("tp", None, None),
        P("tp"),
        P(),
        P(("sp", "tp"), None),
        P(("sp", "tp"), None),
        P("sp", None, "tp"),
        P("sp", None, "tp"),
        P("sp", "tp", None),
    )
    out_specs = P(("sp", "tp"), None)
    return jax.shard_map(
        per_device, mesh=mesh, in_specs=in_specs, out_specs=out_specs, check_vma=False
    )
```
